256 devices in a mesh: ep: 64 (over z, y, core), tp: 4 (over x).
Axes of the slice: x: 4, y: 4, z: 8, core: 2. Of those that a mesh axis runs over, the one named last changes fastest.
Arguments:
- queries: bfloat16 [32768, 2048], P('ep', 'tp'), may hold values from -6 to 6
- forget_pre: float32 [32768, 2048], P('ep', 'tp'), may hold values from -8 to 20
- value_in: bfloat16 [32768, 2048], P('ep', 'tp'), may hold values from -6 to 6
- out_gate: bfloat16 [32768, 2048], P('ep', 'tp'), may hold values from -6 to 6
- lower_bound: float32 [2048], P('tp'), may hold values from 0.5 to 0.8
- out_gain: float32 [128], replicated, may hold values from 0.1 to 1.9
- out_weight: bfloat16 [2048, 2048], P('tp'), may hold values from -0.125 to 0.125
- moe_tokens: bfloat16 [16384, 2048], P('ep'), may hold values from -6 to 6
- moe_gain: float32 [2048], replicated, may hold values from 0.1 to 1.9
- expert_ids: int32 [16384, 4], P('ep'), may hold values from 0 to 127, all different within a row; in each aligned block of 64 rows (0 to 63, 64 to 127, ...) at most 4 rows name the same one
- route_weights: float32 [16384, 4], P('ep'), may hold values from 0.1 to 1
- w_gate: bfloat16 [128, 2048, 1024], P('ep', None, 'tp'), may hold values from -0.125 to 0.125
- w_up: bfloat16 [128, 2048, 1024], P('ep', None, 'tp'), may hold values from -0.125 to 0.125
- w_down: bfloat16 [128, 1024, 2048], P('ep', 'tp'), may hold values from -0.1875 to 0.1875
Outputs:
- mixer_out: bfloat16 [32768, 2048], P(('ep', 'tp'))
- expert_out: bfloat16 [16384, 2048], P(('ep', 'tp'))
The draws below stay inside these ranges and needn't reach their ends.
Inputs may be any that keep to these rules, and one draw needn't show every extreme that they name: `expert_ids`: each row names 4 different experts. In each aligned block of 64 rows no expert is named by more than 4 rows, and in some block some expert is named by exactly 4 rows.
All inputs are finite; a program needn't handle non-finite values.
Results may differ from the reference program's by a relative error of at most 0.01065.
Values may be sent and summed in bfloat16 or wider, within the bound.
No kernel may reach another device: no remote copies, remote signals or barrier semaphores. Data moves between devices by JAX's collectives and lax.ppermute only.
A program may use at most 128 MiB of HBM per device.

```python
import math
import jax
import jax.numpy as jnp
import numpy as np
from jax import lax

D = 2048
HEAD_DIM = 128
BLOCK = 64
FE = 1024
EXPERTS = 128
TOPK = 4
SEQ_DEV = 512
SEQUENCE_TOTAL = 32768
MOE_ALL = 16384
QROWS = 64
CAPQ = 4
N_TP = 4


def draw_forget_pre(key, part):
    random_subkeys = jax.random.split(key, 6)
    slow_share = 0.6
    slow_mask = jax.random.uniform(random_subkeys[0], (D,)) < slow_share
    reach_factor = jax.random.uniform(random_subkeys[1], (D,), minval=0.5, maxval=2.0)
    fast_rate = 1.0 / jax.random.uniform(random_subkeys[2], (D,), minval=30.0, maxval=60.0)
    target = jnp.where(slow_mask, reach_factor / SEQUENCE_TOTAL, fast_rate)
    level_floor = jnp.log(0.35 / target)
    block_shift = jax.random.uniform(random_subkeys[3], (SEQUENCE_TOTAL // SEQ_DEV, 1), minval=-0.7, maxval=0.7)
    level_per_block = jnp.repeat(block_shift, SEQ_DEV, axis=0)
    random_noise = 0.7 * jax.random.truncated_normal(random_subkeys[4], -5.0, 5.0, (SEQUENCE_TOTAL, D))
    spike_events = jax.random.randint(random_subkeys[5], (6,), 0, SEQUENCE_TOTAL)
    position_indices = jnp.arange(SEQUENCE_TOTAL)
    spike_mask = jnp.any(position_indices[:, None] == spike_events[None, :], axis=1)
    sampled_values = jnp.where(spike_mask[:, None], -4.0 + 0.3 * random_noise, level_floor[None, :] + level_per_block + random_noise)
    return sampled_values.astype(jnp.float32)


def shard_levels(rng, extent, cuts, smallest, largest):
    def one(axis_at, parts):
        heights = jax.random.uniform(jax.random.fold_in(jax.random.fold_in(rng, 6), axis_at), (parts,), jnp.float32, smallest / len(cuts), largest / len(cuts))
        return jnp.repeat(jnp.exp(heights), extent[axis_at] // parts).reshape((-1,) + (1,) * (len(extent) - axis_at - 1))

    loudness = one(*cuts[0])
    for cut in cuts[1:]:
        loudness = loudness * one(*cut)
    return loudness


def deal_out(key, own, number, rows, count, top, bound, slope):
    ranking = jax.random.permutation(key, count)
    crowded, ordinary = shares(count, rows * top, bound, slope, True), shares(count, rows * top, bound, slope, False)
    places = jnp.arange(count)

    def named(tallies, turn):
        used = int((tallies > 0).sum())
        fixed = max(1, used // 4)
        shifted = fixed + (places - fixed + turn * (used - fixed)) % max(1, count - fixed)
        return jnp.zeros((count,), jnp.int32).at[ranking[jnp.where(places < fixed, places, shifted)]].set(jnp.asarray(tallies, jnp.int32))

    tallies = jnp.where(number % 4 == 0, named(crowded, number // 4), named(ordinary, number - number // 4 - 1))
    mixed = jax.random.permutation(jax.random.fold_in(own, 3), count)
    donor, receiver = mixed[0:count // 2 * 2:2], mixed[1:count // 2 * 2:2]
    room = jnp.minimum(tallies[donor] - 1, bound - tallies[receiver]) // 2
    room = jnp.where((donor == ranking[0]) | (receiver == ranking[0]) | (tallies[receiver] == 0), 0, jnp.maximum(room, 0))
    shifted = jax.random.randint(jax.random.fold_in(own, 4), (count // 2,), 0, 1 << 20) % (room + 1)
    tallies = tallies.at[donor].add(-shifted).at[receiver].add(shifted)
    members = jnp.searchsorted(jnp.cumsum(tallies), jnp.arange(rows * top), side="right").astype(jnp.int32)
    table = members.reshape(top, rows).T
    table = table[jax.random.permutation(jax.random.fold_in(own, 1), rows)]
    turn = jax.random.randint(jax.random.fold_in(own, 2), (rows, 1), 0, top)
    return jnp.take_along_axis(table, (jnp.arange(top)[None, :] + turn) % top, axis=1)


def shares(amount, total, reach, slope, full):
    portions = [(1 << 20) // math.isqrt(rank ** slope) + 1 for rank in range(1, amount + 1)]
    largest = reach if full else min(reach, max(-(-total // amount), total * portions[0] // sum(portions)))
    least = 1 if total - largest >= amount - 1 else 0
    counts, rest = [largest] + [least] * (amount - 1), total - largest - least * (amount - 1)
    while rest > 0:
        candidates = [i for i in range(1, amount) if counts[i] < largest] or [i for i in range(1, amount) if counts[i] < reach]
        pool, left = sum([portions[i] for i in candidates]), rest
        for i in candidates:
            more = min(reach - counts[i], max(1, left * portions[i] // pool), rest)
            counts[i] = counts[i] + more
            rest = rest - more
    return np.array(counts)


def gaussian(key, extent, spread, most, cuts=(), kind=jnp.bfloat16):
    entries = jax.random.normal(key, extent, jnp.float32) * spread
    if len(cuts) > 0:
        entries = shard_levels(key, extent, cuts, -0.22, 0.18) * entries
    return jnp.clip(entries, min=-most, max=most).astype(kind)


def setup_inputs(seed: int = 0) -> dict:
    seeds = jax.random.split(jax.random.key(seed), 15)
    queries = gaussian(seeds[0], (SEQUENCE_TOTAL, D), 1.0, 6.0, ((0, 64), (1, 4)))
    forget_pre = draw_forget_pre(jax.random.fold_in(seeds[14], 71), 0)
    value_in = gaussian(seeds[2], (SEQUENCE_TOTAL, D), 1.0, 6.0, ((0, 64), (1, 4)))
    out_gate = gaussian(seeds[3], (SEQUENCE_TOTAL, D), 1.0, 6.0, ((0, 64), (1, 4)))
    lower_bound = jnp.clip(0.5 + 0.3 * jax.random.uniform(seeds[4], (D,), jnp.float32) ** shard_levels(seeds[4], (D,), ((0, 4),), -0.2, 0.2), 0.5, 0.8)
    out_gain = jnp.clip(1.0 + 0.18 * jax.random.normal(seeds[5], (HEAD_DIM,), jnp.float32), 0.1, 1.9)
    out_weight = gaussian(seeds[6], (D, D), D ** -0.5, 0.125, ((0, 4),))
    moe_tokens = gaussian(seeds[7], (MOE_ALL, D), 1.0, 6.0, ((0, 64),))
    moe_gain = jnp.clip(1.0 + 0.18 * jax.random.normal(seeds[8], (D,), jnp.float32), 0.1, 1.9)
    expert_ids_keys = jax.random.split(jax.random.fold_in(seeds[9], 1), MOE_ALL // QROWS)
    expert_ids_turns = jax.random.permutation(jax.random.fold_in(seeds[9], 3), MOE_ALL // QROWS)
    expert_ids = jax.vmap(lambda own, number: deal_out(jax.random.fold_in(seeds[9], 2), own, number, QROWS, EXPERTS, TOPK, CAPQ, 2))(expert_ids_keys, expert_ids_turns).reshape((MOE_ALL, TOPK))
    route_weights = jnp.clip(jnp.exp(math.log(1.0) - 2.3025851 * jax.random.uniform(seeds[10], (MOE_ALL, TOPK), jnp.float32) ** shard_levels(seeds[10], (MOE_ALL, TOPK), ((0, 64),), -0.2, 0.2)), 0.1, 1.0)
    w_gate = gaussian(seeds[11], (EXPERTS, D, FE), D ** -0.5, 0.125, ((0, 64), (2, 4)))
    w_up = gaussian(seeds[12], (EXPERTS, D, FE), D ** -0.5, 0.125, ((0, 64), (2, 4)))
    w_down = gaussian(seeds[13], (EXPERTS, FE, D), FE ** -0.5, 0.1875, ((0, 64), (1, 4)))
    return dict(queries=queries, forget_pre=forget_pre, value_in=value_in, out_gate=out_gate, lower_bound=lower_bound, out_gain=out_gain, out_weight=out_weight, moe_tokens=moe_tokens, moe_gain=moe_gain, expert_ids=expert_ids, route_weights=route_weights, w_gate=w_gate, w_up=w_up, w_down=w_down)


EPS = 1e-06
HIGHEST = lax.Precision.HIGHEST

def rms_scale(values, gain):
    return values * lax.rsqrt(lax.optimization_barrier(jnp.mean(values * values, axis=-1, keepdims=True)) + EPS) * gain

def block_step(memory, inputs):
    queries_block, weight_block, values_block, forget_block = inputs
    cumulative = jnp.cumsum(forget_block, axis=1)
    length = queries_block.shape[1]
    causal = jnp.arange(length, dtype=jnp.int32)[:, None] >= jnp.arange(length, dtype=jnp.int32)[None, :]
    decayed_query = queries_block * jnp.exp(cumulative)
    decayed_key = weight_block * jnp.exp(-cumulative)
    carried_out = jnp.einsum('htd,hde->hte', decayed_query, memory, precision=HIGHEST)
    scores = jnp.einsum('htd,hsd->hts', decayed_query, decayed_key, precision=HIGHEST)
    scores = jnp.where(causal[None], scores, 0.0)
    local_out = jnp.einsum('hts,hse->hte', scores, values_block, precision=HIGHEST)
    block_total = cumulative[:, -1:, :]
    added = jnp.einsum('hsd,hse->hde', weight_block * jnp.exp(block_total - cumulative), values_block, precision=HIGHEST)
    memory = jnp.exp(block_total[:, 0, :])[:, :, None] * memory + added
    return (memory, carried_out + local_out)

def to_blocks(array, head_count):
    row_count = array.shape[0]
    return array.astype(jnp.float32).reshape(row_count // BLOCK, BLOCK, head_count, HEAD_DIM).transpose(0, 2, 1, 3)

def mixer_part(queries, forget_pre, value_in, out_gate, lower_bound, out_gain, out_weight):
    seq_rows, model_width = queries.shape
    head_count = model_width // HEAD_DIM
    weight_in = (1.0 - lower_bound) * jax.nn.sigmoid(-forget_pre)
    log_forget = jnp.log1p(-weight_in)
    start_memory = jnp.zeros((head_count, HEAD_DIM, HEAD_DIM), jnp.float32)
    final_memory, outputs = lax.scan(block_step, start_memory, (to_blocks(queries, head_count), to_blocks(weight_in, head_count), to_blocks(value_in, head_count), to_blocks(log_forget, head_count)))
    outputs = outputs.transpose(0, 2, 1, 3).reshape(seq_rows, head_count, HEAD_DIM)
    gate_act = jax.nn.silu(out_gate.astype(jnp.float32)).reshape(seq_rows, head_count, HEAD_DIM)
    gated = (rms_scale(outputs, out_gain) * gate_act).reshape(seq_rows, model_width).astype(jnp.bfloat16)
    group_width = model_width // N_TP
    summed = jnp.zeros((seq_rows, model_width), jnp.float32)
    for group_index in range(N_TP):
        low = group_index * group_width
        partial_value = jnp.dot(gated[:, low:low + group_width], out_weight[low:low + group_width], preferred_element_type=jnp.float32)
        summed = summed + lax.optimization_barrier(partial_value.astype(jnp.bfloat16)).astype(jnp.float32)
    return summed.astype(jnp.bfloat16)

def slot_ranks(ids_block, expert_count):
    onehot = (ids_block[:, :, None] == jnp.arange(expert_count, dtype=jnp.int32)[None, None, :]).astype(jnp.int32)
    return lax.optimization_barrier(jnp.sum(onehot * (jnp.cumsum(onehot, axis=1) - 1), axis=2)).astype(jnp.int32)

def experts_part(moe_tokens, moe_gain, expert_ids, route_weights, w_gate, w_up, w_down):
    token_count, model_width = moe_tokens.shape
    expert_count = w_gate.shape[0]
    hidden_units = w_gate.shape[2]
    top_count = expert_ids.shape[1]
    normed = rms_scale(moe_tokens.astype(jnp.float32), moe_gain).astype(jnp.bfloat16)
    padded = jnp.concatenate([normed, jnp.zeros((1, model_width), jnp.bfloat16)], axis=0)
    block_count = token_count // QROWS
    ids_block = expert_ids.astype(jnp.int32).reshape(block_count, QROWS * top_count)
    ranks = slot_ranks(ids_block, expert_count)
    block_base = jnp.arange(block_count, dtype=jnp.int32)[:, None] * CAPQ
    columns = (block_base + ranks).reshape(-1)
    flat_ids = ids_block.reshape(-1)
    token_index = jnp.arange(token_count * top_count, dtype=jnp.int32) // top_count
    table = jnp.full((expert_count, block_count * CAPQ), token_count, jnp.int32).at[flat_ids, columns].set(token_index)
    weight_table = jnp.zeros((expert_count, block_count * CAPQ), jnp.float32).at[flat_ids, columns].set(route_weights.reshape(-1))
    group_units = hidden_units // N_TP

    def one_expert(summed, inputs):
        rows_index, weights_now, gate_matrix, up_matrix, down_matrix = inputs
        rows_now = padded[rows_index]
        gate_pre = jnp.dot(rows_now, gate_matrix, preferred_element_type=jnp.float32)
        up_pre = jnp.dot(rows_now, up_matrix, preferred_element_type=jnp.float32)
        hidden = (jax.nn.silu(gate_pre) * up_pre).astype(jnp.bfloat16)
        total_rows = jnp.zeros((rows_now.shape[0], model_width), jnp.float32)
        for group_index in range(N_TP):
            low = group_index * group_units
            partial_value = jnp.dot(hidden[:, low:low + group_units], down_matrix[low:low + group_units], preferred_element_type=jnp.float32)
            total_rows = total_rows + lax.optimization_barrier(partial_value.astype(jnp.bfloat16)).astype(jnp.float32)
        expert_rows = lax.optimization_barrier(total_rows.astype(jnp.bfloat16)).astype(jnp.float32)
        return (summed.at[rows_index].add(expert_rows * weights_now[:, None]), None)
    start_sum = jnp.zeros((token_count + 1, model_width), jnp.float32)
    summed, unused = lax.scan(one_expert, start_sum, (table, weight_table, w_gate, w_up, w_down))
    return summed[:token_count].astype(jnp.bfloat16)

def reference(queries, forget_pre, value_in, out_gate, lower_bound, out_gain, out_weight, moe_tokens, moe_gain, expert_ids, route_weights, w_gate, w_up, w_down):
    mixer_out = mixer_part(queries, forget_pre, value_in, out_gate, lower_bound, out_gain, out_weight)
    expert_out = experts_part(moe_tokens, moe_gain, expert_ids, route_weights, w_gate, w_up, w_down)
    return (mixer_out, expert_out)
```

```python
import functools

import jax
import jax.numpy as jnp
from jax import lax
from jax.experimental import pallas as pl
from jax.experimental.pallas import tpu as pltpu
from jax.sharding import Mesh
from jax.sharding import PartitionSpec as P

HEAD_DIM = 128
BLOCK = 64
CAP = 4
CHUNKS = 4
EP = ("ep_0", "ep_1", "ep_2")
EP_TP = ("ep_0", "ep_1", "ep_2", "tp")

EPS = 1e-06
HIGHEST = lax.Precision.HIGHEST


def shifted(x, by):
    count = lax.axis_size("tp")
    return lax.ppermute(x, "tp", [(i, (i + by) % count) for i in range(count)])


def rms_scale(values, gain):
    return values * lax.rsqrt(jnp.mean(values * values, axis=-1, keepdims=True) + EPS) * gain


def dot_nt(a, b, precision=HIGHEST):
    return lax.dot_general(
        a, b, (((1,), (1,)), ((), ())), precision=precision, preferred_element_type=jnp.float32
    )


def dot_tn(a, b, precision=HIGHEST):
    return lax.dot_general(
        a, b, (((0,), (0,)), ((), ())), precision=precision, preferred_element_type=jnp.float32
    )


def dot_nn(a, b, precision=HIGHEST):
    return lax.dot_general(
        a, b, (((1,), (0,)), ((), ())), precision=precision, preferred_element_type=jnp.float32
    )


def recurrence_kernel(q_ref, f_ref, v_ref, bound_ref, rec_ref, query_ref, state_ref, decay_ref):
    rows = q_ref.shape[0]
    row = lax.broadcasted_iota(jnp.int32, (BLOCK, BLOCK), 0)
    col = lax.broadcasted_iota(jnp.int32, (BLOCK, BLOCK), 1)
    causal = row >= col
    lower = causal.astype(jnp.float32)
    scale = 1.0 - bound_ref[0]

    def step(b, carry):
        state, before = carry
        here = pl.ds(pl.multiple_of(b * BLOCK, BLOCK), BLOCK)
        weight = scale * jax.nn.sigmoid(-f_ref[here, :])
        log_forget = jnp.log1p(-weight)
        cumulative = dot_nn(lower, log_forget)
        queries = q_ref[here, :].astype(jnp.float32)
        values = v_ref[here, :].astype(jnp.float32)
        decayed_query = queries * jnp.exp(cumulative)
        decayed_key = weight * jnp.exp(-cumulative)
        scores = jnp.where(causal, dot_nt(decayed_query, decayed_key), 0.0)
        rec_ref[here, :] = dot_nt(decayed_query, state) + dot_nn(scores, values)
        query_ref[here, :] = queries * jnp.exp(cumulative + before)
        total = cumulative[BLOCK - 1 :, :]
        state = jnp.exp(total) * state + dot_tn(values, weight * jnp.exp(total - cumulative))
        return state, before + total

    state, total = lax.fori_loop(
        0,
        rows // BLOCK,
        step,
        (jnp.zeros((HEAD_DIM, HEAD_DIM), jnp.float32), jnp.zeros((1, HEAD_DIM), jnp.float32)),
    )
    state_ref[0] = state
    decay_ref[0] = jnp.broadcast_to(jnp.exp(total), decay_ref.shape[1:])


def recurrence(queries, forget_pre, value_in, lower_bound):
    rows, width = queries.shape
    heads = width // HEAD_DIM
    wide = pl.BlockSpec((rows, HEAD_DIM), lambda h: (0, h))
    return pl.pallas_call(
        recurrence_kernel,
        grid=(heads,),
        in_specs=[wide, wide, wide, pl.BlockSpec((1, 1, HEAD_DIM), lambda h: (h, 0, 0))],
        out_specs=[
            wide,
            wide,
            pl.BlockSpec((1, HEAD_DIM, HEAD_DIM), lambda h: (h, 0, 0)),
            pl.BlockSpec((1, 8, HEAD_DIM), lambda h: (h, 0, 0)),
        ],
        out_shape=[
            jax.ShapeDtypeStruct((rows, width), jnp.float32),
            jax.ShapeDtypeStruct((rows, width), jnp.float32),
            jax.ShapeDtypeStruct((heads, HEAD_DIM, HEAD_DIM), jnp.float32),
            jax.ShapeDtypeStruct((heads, 8, HEAD_DIM), jnp.float32),
        ],
        name="recurrence",
    )(queries, forget_pre, value_in, lower_bound.reshape(heads, 1, HEAD_DIM))


def prefix_kernel(pieces_ref, out_ref):
    def step(k, before):
        out_ref[k] = before
        return before * pieces_ref[k, 8:, :] + pieces_ref[k, :8, :]

    lax.fori_loop(0, pieces_ref.shape[0], step, jnp.zeros(out_ref.shape[1:], jnp.float32))


def prefix(pieces):
    return pl.pallas_call(
        prefix_kernel,
        out_shape=jax.ShapeDtypeStruct((pieces.shape[0], 8, HEAD_DIM), jnp.float32),
        name="prefix",
    )(pieces)


def gate_kernel(rec_ref, query_ref, state_ref, out_gate_ref, gain_ref, out_ref):
    rec = rec_ref[...] + dot_nt(query_ref[...], state_ref[0])
    act = jax.nn.silu(out_gate_ref[...].astype(jnp.float32))
    out_ref[...] = (rms_scale(rec, gain_ref[...]) * act).astype(jnp.bfloat16)


def gate(rec, query, state, out_gate, out_gain):
    rows, width = rec.shape
    wide = pl.BlockSpec((rows, HEAD_DIM), lambda h: (0, h))
    return pl.pallas_call(
        gate_kernel,
        grid=(width // HEAD_DIM,),
        in_specs=[
            wide,
            wide,
            pl.BlockSpec((1, HEAD_DIM, HEAD_DIM), lambda h: (h, 0, 0)),
            wide,
            pl.BlockSpec((1, HEAD_DIM), lambda h: (0, 0)),
        ],
        out_specs=wide,
        out_shape=jax.ShapeDtypeStruct((rows, width), jnp.bfloat16),
        name="gate",
    )(rec, query, state, out_gate, out_gain.reshape(1, HEAD_DIM))


def mixer(queries, forget_pre, value_in, out_gate, lower_bound, out_gain, out_weight):
    heads = queries.shape[1] // HEAD_DIM
    spans = lax.axis_size(EP)
    lanes = lax.axis_size("tp")
    rec, query, state, decay = recurrence(queries, forget_pre, value_in, lower_bound)
    per_head = spans // heads
    decays = jnp.broadcast_to(decay[:, None], (heads, per_head, 8, HEAD_DIM))
    leaving = jnp.concatenate(
        [
            state.reshape(spans, heads * HEAD_DIM // spans, HEAD_DIM),
            decays.reshape(spans, 8, HEAD_DIM),
        ],
        axis=1,
    )
    pieces = lax.all_to_all(leaving, EP, split_axis=0, concat_axis=0, tiled=True)
    starts = lax.all_to_all(prefix(pieces), EP, split_axis=0, concat_axis=0, tiled=True)
    gated = gate(rec, query, starts.reshape(heads, HEAD_DIM, HEAD_DIM), out_gate, out_gain)
    parts = jnp.dot(gated, out_weight, preferred_element_type=jnp.float32).astype(jnp.bfloat16)
    parts = parts.reshape(lanes, parts.shape[0] // lanes, -1)
    arrived = lax.all_to_all(parts, "tp", split_axis=0, concat_axis=0, tiled=True)
    return arrived.astype(jnp.float32).sum(axis=0).astype(jnp.bfloat16)


def first_expert(shape):
    row = lax.broadcasted_iota(jnp.int32, shape, 0)
    return row % (2 * CAP) < CAP


def hidden_kernel(*refs):
    row_refs, (gate_ref, up_ref, out_ref) = refs[:-3], refs[-3:]
    width = row_refs[0].shape[1]

    def product(weight_ref, expert):
        total = None
        for k, ref in enumerate(row_refs):
            part = dot_nn(ref[...], weight_ref[expert, k * width : (k + 1) * width, :], None)
            total = part if total is None else total + part
        return total

    first = first_expert(out_ref.shape)
    gate_pre = jnp.where(first, product(gate_ref, 0), product(gate_ref, 1))
    up_pre = jnp.where(first, product(up_ref, 0), product(up_ref, 1))
    out_ref[...] = (jax.nn.silu(gate_pre) * up_pre).astype(jnp.bfloat16)


def hidden_units(row_pieces, w_gate, w_up, tile=256):
    rows, width = row_pieces[0].shape
    units = w_gate.shape[2]
    whole = pl.BlockSpec(w_gate.shape, lambda r: (0, 0, 0))
    return pl.pallas_call(
        hidden_kernel,
        grid=(rows // tile,),
        in_specs=[pl.BlockSpec((tile, width), lambda r: (r, 0))] * len(row_pieces) + [whole, whole],
        out_specs=pl.BlockSpec((tile, units), lambda r: (r, 0)),
        out_shape=jax.ShapeDtypeStruct((rows, units), jnp.bfloat16),
        name="hidden_units",
    )(*row_pieces, w_gate, w_up)


def down_kernel(*refs):
    out_ref = refs[-1]
    count = (len(refs) - 1) // 2
    hidden_refs, weight_refs = refs[:count], refs[count:-1]

    def product(expert):
        total = None
        for ref, weight_ref in zip(hidden_refs, weight_refs):
            part = dot_nn(ref[...], weight_ref[expert], None)
            total = part if total is None else total + part
        return total

    out_ref[...] = jnp.where(
        first_expert(out_ref.shape), product(0), product(1)
    ).astype(jnp.bfloat16)


def down(hidden_pieces, weight_pieces, tile=256):
    rows, units = hidden_pieces[0].shape
    width = weight_pieces[0].shape[2]
    whole = pl.BlockSpec(weight_pieces[0].shape, lambda r: (0, 0, 0))
    return pl.pallas_call(
        down_kernel,
        grid=(rows // tile,),
        in_specs=[pl.BlockSpec((tile, units), lambda r: (r, 0))] * len(hidden_pieces)
        + [whole] * len(weight_pieces),
        out_specs=pl.BlockSpec((tile, width), lambda r: (r, 0)),
        out_shape=jax.ShapeDtypeStruct((rows, width), jnp.bfloat16),
        name="down",
    )(*hidden_pieces, *weight_pieces)


def slots_filled(ids, expert_count):
    tokens = ids.shape[0]
    slot = jnp.arange(expert_count * CAP, dtype=jnp.int32)
    named = jnp.any(ids.T[:, None, :] == (slot // CAP)[None, :, None], axis=0)
    order = jnp.arange(tokens, dtype=jnp.int32)
    earlier = (order[:, None] < order[None, :]).astype(jnp.bfloat16)
    ranks = jnp.dot(named.astype(jnp.bfloat16), earlier, preferred_element_type=jnp.float32)
    return named & (ranks == (slot % CAP).astype(jnp.float32)[:, None])


def slot_weights(ids, weights, expert_count):
    tokens, top_count = ids.shape
    slot = jnp.arange(expert_count * CAP, dtype=jnp.int32)
    named = ids[:, :, None] == (slot // CAP)[None, None, :]
    weight = jnp.sum(jnp.where(named, weights[:, :, None], 0.0), axis=1)
    named = jnp.any(named, axis=1)
    order = jnp.arange(tokens, dtype=jnp.int32)
    earlier = (order[None, :] < order[:, None]).astype(jnp.bfloat16)
    ranks = jnp.dot(earlier, named.astype(jnp.bfloat16), preferred_element_type=jnp.float32)
    return jnp.where(ranks == (slot % CAP).astype(jnp.float32)[None, :], weight, 0.0)


def experts(moe_tokens, moe_gain, expert_ids, route_weights, w_gate, w_up, w_down):
    lanes = lax.axis_size("tp")
    lane = lax.axis_index("tp")
    ep_count = lax.axis_size(EP)
    local_experts, model_width, _ = w_gate.shape
    expert_count = local_experts * ep_count
    qrows = moe_tokens.shape[0] // lanes
    per_device = local_experts * CAP
    slots = expert_count * CAP
    quarter_width = model_width // lanes

    def from_lane(x, dim):
        twice = jnp.concatenate([x, x], axis=dim)
        start = lane * (x.shape[dim] // lanes)
        return lax.dynamic_slice_in_dim(twice, start, x.shape[dim], dim)

    down_weights = [
        lax.dynamic_slice_in_dim(w_down, (lane + s) % lanes * quarter_width, quarter_width, 2)
        for s in range(lanes)
    ]
    down_weights = [down_weights[0]] + [shifted(down_weights[s], s) for s in range(1, lanes)]

    ids = from_lane(expert_ids, 0).reshape(lanes, qrows, -1)
    weights = from_lane(route_weights, 0).reshape(lanes, qrows, -1)
    tokens = lax.dynamic_slice_in_dim(moe_tokens, lane * qrows, qrows, 0)
    normed = rms_scale(tokens.astype(jnp.float32), moe_gain).astype(jnp.bfloat16)
    filled = slots_filled(ids[0], expert_count).astype(jnp.bfloat16)

    width = model_width // CHUNKS
    rows = [[None] * CHUNKS for _ in range(lanes)]
    for k in range(CHUNKS):
        outgoing = jnp.dot(
            filled, normed[:, k * width : (k + 1) * width], preferred_element_type=jnp.float32
        ).astype(jnp.bfloat16)
        own = lax.all_to_all(
            outgoing.reshape(ep_count, per_device, width), EP, 0, 0, tiled=True
        ).reshape(slots, width)
        rows[0][k] = own
        rows[3][k] = shifted(own, 1)
        rows[1][k] = shifted(own, -1)
        rows[2][k] = shifted(rows[3][k], 1) if k % 2 == 0 else shifted(rows[1][k], -1)

    hidden = [hidden_units(rows[r], w_gate, w_up) for r in range(lanes)]

    combined = []
    for r in range(lanes):
        before = shifted(hidden[(r + 1) % 4], 1)
        after = shifted(hidden[(r + 3) % 4], -1)
        combined.append([hidden[r], before, None, after])
    for r in range(lanes):
        if r % 2 == 0:
            combined[r][2] = shifted(combined[(r + 1) % 4][1], 1)
        else:
            combined[r][2] = shifted(combined[(r + 3) % 4][3], -1)

    outs = []
    for r in range(lanes):
        leaving = down(combined[r], down_weights)
        returned = lax.all_to_all(
            leaving.reshape(ep_count, per_device, quarter_width), EP, 0, 0, tiled=True
        ).reshape(slots, quarter_width)
        mix = slot_weights(ids[r], weights[r], expert_count)
        high = lax.reduce_precision(mix, 8, 7)
        out = jnp.dot(
            high.astype(jnp.bfloat16), returned, preferred_element_type=jnp.float32
        ) + jnp.dot(
            (mix - high).astype(jnp.bfloat16), returned, preferred_element_type=jnp.float32
        )
        outs.append(out.astype(jnp.bfloat16))
    arrived = [outs[0]] + [shifted(outs[s], s) for s in range(1, lanes)]
    ordered = jnp.stack(arrived[::-1] + arrived[::-1])
    ordered = lax.dynamic_slice_in_dim(ordered, (lanes - 1 - lane) % lanes, lanes, 0)
    return ordered.transpose(1, 0, 2).reshape(qrows, model_width)


def local(
    queries,
    forget_pre,
    value_in,
    out_gate,
    lower_bound,
    out_gain,
    out_weight,
    moe_tokens,
    moe_gain,
    expert_ids,
    route_weights,
    w_gate,
    w_up,
    w_down,
):
    expert_out = experts(
        moe_tokens, moe_gain, expert_ids, route_weights, w_gate, w_up, w_down
    )
    mixer_out = mixer(
        queries, forget_pre, value_in, out_gate, lower_bound, out_gain, out_weight
    )
    return mixer_out, expert_out


def solution(mesh):
    split = Mesh(mesh.devices.reshape(8, 4, 2, mesh.shape["tp"]), ("ep_0", "ep_1", "ep_2", "tp"))
    placed = (
        P(EP, "tp"),
        P(EP, "tp"),
        P(EP, "tp"),
        P(EP, "tp"),
        P("tp"),
        P(),
        P("tp", None),
        P(EP, None),
        P(),
        P(EP, None),
        P(EP, None),
        P(EP, None, "tp"),
        P(EP, None, "tp"),
        P(EP, "tp", None),
    )
    return jax.shard_map(
        local,
        mesh=split,
        in_specs=placed,
        out_specs=(P(EP_TP, None), P(EP_TP, None)),
        check_vma=False,
    )
```

```python
import functools

import jax
import jax.numpy as jnp
from jax import lax
from jax.experimental import pallas as pl
from jax.experimental.pallas import tpu as pltpu
from jax.sharding import Mesh
from jax.sharding import PartitionSpec as P

HEAD_DIM = 128
BLOCK = 64
CAP = 4
EP = ("ep_0", "ep_1", "ep_2")
EP_TP = ("ep_0", "ep_1", "ep_2", "tp")

EPS = 1e-06
HIGHEST = lax.Precision.HIGHEST


def rms_scale(values, gain):
    return values * lax.rsqrt(jnp.mean(values * values, axis=-1, keepdims=True) + EPS) * gain


def dot_nt(a, b, precision=HIGHEST):
    return lax.dot_general(
        a, b, (((1,), (1,)), ((), ())), precision=precision, preferred_element_type=jnp.float32
    )


def dot_tn(a, b, precision=HIGHEST):
    return lax.dot_general(
        a, b, (((0,), (0,)), ((), ())), precision=precision, preferred_element_type=jnp.float32
    )


def dot_nn(a, b, precision=HIGHEST):
    return lax.dot_general(
        a, b, (((1,), (0,)), ((), ())), precision=precision, preferred_element_type=jnp.float32
    )


def recurrence_kernel(q_ref, f_ref, v_ref, bound_ref, rec_ref, query_ref, state_ref, decay_ref):
    rows = q_ref.shape[0]
    row = lax.broadcasted_iota(jnp.int32, (BLOCK, BLOCK), 0)
    col = lax.broadcasted_iota(jnp.int32, (BLOCK, BLOCK), 1)
    causal = row >= col
    lower = causal.astype(jnp.float32)
    scale = 1.0 - bound_ref[0]

    def step(b, carry):
        state, before = carry
        here = pl.ds(pl.multiple_of(b * BLOCK, BLOCK), BLOCK)
        weight = scale * jax.nn.sigmoid(-f_ref[here, :])
        log_forget = jnp.log1p(-weight)
        cumulative = dot_nn(lower, log_forget)
        queries = q_ref[here, :].astype(jnp.float32)
        values = v_ref[here, :].astype(jnp.float32)
        decayed_query = queries * jnp.exp(cumulative)
        decayed_key = weight * jnp.exp(-cumulative)
        scores = jnp.where(causal, dot_nt(decayed_query, decayed_key), 0.0)
        rec_ref[here, :] = dot_nt(decayed_query, state) + dot_nn(scores, values)
        query_ref[here, :] = queries * jnp.exp(cumulative + before)
        total = cumulative[BLOCK - 1 :, :]
        state = jnp.exp(total) * state + dot_tn(values, weight * jnp.exp(total - cumulative))
        return state, before + total

    state, total = lax.fori_loop(
        0,
        rows // BLOCK,
        step,
        (jnp.zeros((HEAD_DIM, HEAD_DIM), jnp.float32), jnp.zeros((1, HEAD_DIM), jnp.float32)),
    )
    state_ref[0] = state
    decay_ref[0] = jnp.broadcast_to(jnp.exp(total), decay_ref.shape[1:])


def recurrence(queries, forget_pre, value_in, lower_bound):
    rows, width = queries.shape
    heads = width // HEAD_DIM
    wide = pl.BlockSpec((rows, HEAD_DIM), lambda h: (0, h))
    return pl.pallas_call(
        recurrence_kernel,
        grid=(heads,),
        in_specs=[wide, wide, wide, pl.BlockSpec((1, 1, HEAD_DIM), lambda h: (h, 0, 0))],
        out_specs=[
            wide,
            wide,
            pl.BlockSpec((1, HEAD_DIM, HEAD_DIM), lambda h: (h, 0, 0)),
            pl.BlockSpec((1, 8, HEAD_DIM), lambda h: (h, 0, 0)),
        ],
        out_shape=[
            jax.ShapeDtypeStruct((rows, width), jnp.float32),
            jax.ShapeDtypeStruct((rows, width), jnp.float32),
            jax.ShapeDtypeStruct((heads, HEAD_DIM, HEAD_DIM), jnp.float32),
            jax.ShapeDtypeStruct((heads, 8, HEAD_DIM), jnp.float32),
        ],
        name="recurrence",
    )(queries, forget_pre, value_in, lower_bound.reshape(heads, 1, HEAD_DIM))


def prefix_kernel(pieces_ref, out_ref):
    def step(k, before):
        out_ref[k] = before
        return before * pieces_ref[k, 8:, :] + pieces_ref[k, :8, :]

    lax.fori_loop(0, pieces_ref.shape[0], step, jnp.zeros(out_ref.shape[1:], jnp.float32))


def prefix(pieces):
    return pl.pallas_call(
        prefix_kernel,
        out_shape=jax.ShapeDtypeStruct((pieces.shape[0], 8, HEAD_DIM), jnp.float32),
        name="prefix",
    )(pieces)


def gate_kernel(rec_ref, query_ref, state_ref, out_gate_ref, gain_ref, out_ref):
    rec = rec_ref[...] + dot_nt(query_ref[...], state_ref[0])
    act = jax.nn.silu(out_gate_ref[...].astype(jnp.float32))
    out_ref[...] = (rms_scale(rec, gain_ref[...]) * act).astype(jnp.bfloat16)


def gate(rec, query, state, out_gate, out_gain):
    rows, width = rec.shape
    wide = pl.BlockSpec((rows, HEAD_DIM), lambda h: (0, h))
    return pl.pallas_call(
        gate_kernel,
        grid=(width // HEAD_DIM,),
        in_specs=[
            wide,
            wide,
            pl.BlockSpec((1, HEAD_DIM, HEAD_DIM), lambda h: (h, 0, 0)),
            wide,
            pl.BlockSpec((1, HEAD_DIM), lambda h: (0, 0)),
        ],
        out_specs=wide,
        out_shape=jax.ShapeDtypeStruct((rows, width), jnp.bfloat16),
        name="gate",
    )(rec, query, state, out_gate, out_gain.reshape(1, HEAD_DIM))


def mixer(queries, forget_pre, value_in, out_gate, lower_bound, out_gain, out_weight):
    heads = queries.shape[1] // HEAD_DIM
    spans = lax.axis_size(EP)
    lanes = lax.axis_size("tp")
    rec, query, state, decay = recurrence(queries, forget_pre, value_in, lower_bound)
    per_head = spans // heads
    decays = jnp.broadcast_to(decay[:, None], (heads, per_head, 8, HEAD_DIM))
    leaving = jnp.concatenate(
        [
            state.reshape(spans, heads * HEAD_DIM // spans, HEAD_DIM),
            decays.reshape(spans, 8, HEAD_DIM),
        ],
        axis=1,
    )
    pieces = lax.all_to_all(leaving, EP, split_axis=0, concat_axis=0, tiled=True)
    starts = lax.all_to_all(prefix(pieces), EP, split_axis=0, concat_axis=0, tiled=True)
    gated = gate(rec, query, starts.reshape(heads, HEAD_DIM, HEAD_DIM), out_gate, out_gain)
    parts = jnp.dot(gated, out_weight, preferred_element_type=jnp.float32).astype(jnp.bfloat16)
    parts = parts.reshape(lanes, parts.shape[0] // lanes, -1)
    arrived = lax.all_to_all(parts, "tp", split_axis=0, concat_axis=0, tiled=True)
    return arrived.astype(jnp.float32).sum(axis=0).astype(jnp.bfloat16)


def expert_kernel(core_ref, *refs):
    sets, steps = 2, 4
    row_refs = refs[:sets]
    sources = refs[sets : sets + 4 * steps]
    out_refs = refs[sets + 4 * steps : 2 * sets + 4 * steps]
    in_buffer, out_buffer, sum_ref, sems = refs[2 * sets + 4 * steps :]
    rows = row_refs[0].shape[0]
    half = out_buffer.shape[2]

    def copy(step, kind):
        buffer = in_buffer if kind < 2 else out_buffer
        place = 2 * step + kind % 2
        return pltpu.make_async_copy(
            sources[kind * steps + step], buffer.at[place], sems.at[4 * step + kind]
        )

    for step in range(steps):
        for kind in range(4):
            copy(step, kind).start()
    gate_is_own = core_ref[0] == 0
    for step in range(steps):
        for kind in range(4):
            copy(step, kind).wait()
        for s in range(sets):
            here = slice(s * rows, (s + 1) * rows)
            own = dot_nn(row_refs[s][...], in_buffer[2 * step], None)
            other = dot_nn(row_refs[s][...], in_buffer[2 * step + 1], None)
            gate_pre = jnp.where(gate_is_own, own, other)
            up_pre = jnp.where(gate_is_own, other, own)
            hidden = (jax.nn.silu(gate_pre) * up_pre).astype(jnp.bfloat16)
            for side in range(2):
                part = dot_nn(hidden, out_buffer[2 * step + side], None)
                if step > 0:
                    part = part + sum_ref[side, here, :]
                sum_ref[side, here, :] = part
    for s in range(sets):
        here = slice(s * rows, (s + 1) * rows)
        for side in range(2):
            place = (core_ref[0] if side == 0 else 1 - core_ref[0]) * half
            out_refs[s][:, pl.ds(pl.multiple_of(place, half), half)] = sum_ref[
                side, here, :
            ].astype(jnp.bfloat16)


def expert_rows(core, row_sets, own_in, other_in, own_out, other_out):
    rows, width = row_sets[0].shape
    units = own_in[0].shape[1]
    half = own_out[0].shape[1]
    vmem = pl.BlockSpec(memory_space=pltpu.VMEM)
    hbm = pl.BlockSpec(memory_space=pl.ANY)
    return pl.pallas_call(
        expert_kernel,
        in_specs=[pl.BlockSpec(memory_space=pltpu.SMEM)] + [vmem] * 2 + [hbm] * 16,
        out_specs=[vmem] * 2,
        out_shape=[jax.ShapeDtypeStruct((rows, width), jnp.bfloat16)] * 2,
        scratch_shapes=[
            pltpu.VMEM((8, width, units), jnp.bfloat16),
            pltpu.VMEM((8, units, half), jnp.bfloat16),
            pltpu.VMEM((2, 2 * rows, half), jnp.float32),
            pltpu.SemaphoreType.DMA((16,)),
        ],
        cost_estimate=pl.CostEstimate(
            flops=12 * 2 * rows * width * 1024, bytes_accessed=24 * 2**20, transcendentals=0
        ),
        name="expert_rows",
    )(core, *row_sets, *own_in, *other_in, *own_out, *other_out)


def slots_filled(ids, slot_count, parity):
    tokens = ids.shape[0]
    slot = jnp.arange(slot_count, dtype=jnp.int32)
    named = jnp.any(ids.T[:, None, :] == (slot // CAP * 2 + parity)[None, :, None], axis=0)
    order = jnp.arange(tokens, dtype=jnp.int32)
    earlier = (order[:, None] < order[None, :]).astype(jnp.bfloat16)
    ranks = jnp.dot(named.astype(jnp.bfloat16), earlier, preferred_element_type=jnp.float32)
    return named & (ranks == (slot % CAP).astype(jnp.float32)[:, None])


def slot_weights(ids, weights, slot_count, parity):
    tokens, top_count = ids.shape
    slot = jnp.arange(slot_count, dtype=jnp.int32)
    named = ids[:, :, None] == (slot // CAP * 2 + parity)[None, None, :]
    weight = jnp.sum(jnp.where(named, weights[:, :, None], 0.0), axis=1)
    named = jnp.any(named, axis=1)
    order = jnp.arange(tokens, dtype=jnp.int32)
    earlier = (order[None, :] < order[:, None]).astype(jnp.bfloat16)
    ranks = jnp.dot(earlier, named.astype(jnp.bfloat16), preferred_element_type=jnp.float32)
    return jnp.where(ranks == (slot % CAP).astype(jnp.float32)[None, :], weight, 0.0)


def weight_moves(turn):
    moves = []
    for core in range(2):
        for lane in range(4):
            piece = lane ^ turn
            moves.append((core * 4 + lane, (piece % 2) * 4 + 2 * core + piece // 2))
    return moves


def row_moves(turn):
    moves = []
    for core in range(2):
        for lane in range(4):
            target = 2 * core + (lane // 2 + turn) % 2
            moves.append((core * 4 + lane, (lane % 2) * 4 + target))
    return moves


RING = ("ep_2", "tp")


def experts(moe_tokens, moe_gain, expert_ids, route_weights, w_gate, w_up, w_down):
    lanes = lax.axis_size("tp")
    lane = lax.axis_index("tp")
    core = lax.axis_index("ep_2")
    ep_count = lax.axis_size(EP)
    model_width = w_gate.shape[1]
    qrows = moe_tokens.shape[0] // lanes
    slots = ep_count * CAP
    half = model_width // 2

    start = lane * qrows
    ids = lax.dynamic_slice_in_dim(expert_ids, start, qrows, 0)
    weights = lax.dynamic_slice_in_dim(route_weights, start, qrows, 0)
    tokens = lax.dynamic_slice_in_dim(moe_tokens, start, qrows, 0)
    normed = rms_scale(tokens.astype(jnp.float32), moe_gain).astype(jnp.bfloat16)
    parities = [(lane // 2 + turn) % 2 for turn in range(2)]

    row_sets = []
    for turn in range(2):
        filled = slots_filled(ids, slots, parities[turn]).astype(jnp.bfloat16)
        leaving = jnp.dot(filled, normed, preferred_element_type=jnp.float32)
        leaving = leaving.astype(jnp.bfloat16).reshape(ep_count, CAP, model_width)
        with jax.named_scope(f"dispatch_{turn}"):
            arrived = lax.all_to_all(leaving, EP, 0, 0, tiled=True)
        with jax.named_scope(f"rows_{turn}"):
            row_sets.append(lax.ppermute(arrived, RING, row_moves(turn)))

    own_in, own_out, other_in, other_out = [], [], [], []
    for turn in range(4):
        piece = lane ^ turn
        expert, part = piece // 2, piece % 2
        gate_now = lax.dynamic_index_in_dim(w_gate, expert, 0, keepdims=False)
        up_now = lax.dynamic_index_in_dim(w_up, expert, 0, keepdims=False)
        in_now = jnp.where(part == 0, gate_now, up_now)
        down_now = lax.dynamic_slice(
            w_down, (expert, 0, part * half), (1, w_down.shape[1], half)
        )[0]
        with jax.named_scope(f"win_{turn}"):
            own_in.append(lax.ppermute(in_now, RING, weight_moves(turn)))
        with jax.named_scope(f"wout_{turn}"):
            own_out.append(lax.ppermute(down_now, RING, weight_moves(turn)))
    for turn in range(4):
        with jax.named_scope(f"swapin_{turn}"):
            other_in.append(lax.ppermute(own_in[turn ^ 1], "ep_2", [(0, 1), (1, 0)]))
        with jax.named_scope(f"swapout_{turn}"):
            other_out.append(lax.ppermute(own_out[turn ^ 1], "ep_2", [(0, 1), (1, 0)]))

    flat = [rows.reshape(slots, model_width) for rows in row_sets]
    results = expert_rows(
        core.astype(jnp.int32).reshape(1), flat, own_in, other_in, own_out, other_out
    )

    total = None
    for turn in range(2):
        leaving = results[turn].reshape(ep_count, CAP, model_width)
        with jax.named_scope(f"back_{turn}"):
            leaving = lax.ppermute(leaving, RING, [(b, a) for a, b in row_moves(turn)])
        with jax.named_scope(f"return_{turn}"):
            returned = lax.all_to_all(leaving, EP, 0, 0, tiled=True)
        returned = returned.reshape(slots, model_width)
        mix = slot_weights(ids, weights, slots, parities[turn])
        high = lax.reduce_precision(mix, 8, 7)
        for factor in (high, mix - high):
            out = jnp.dot(
                factor.astype(jnp.bfloat16), returned, preferred_element_type=jnp.float32
            )
            total = out if total is None else total + out
    return total.astype(jnp.bfloat16)


def local(
    queries,
    forget_pre,
    value_in,
    out_gate,
    lower_bound,
    out_gain,
    out_weight,
    moe_tokens,
    moe_gain,
    expert_ids,
    route_weights,
    w_gate,
    w_up,
    w_down,
):
    expert_out = experts(
        moe_tokens, moe_gain, expert_ids, route_weights, w_gate, w_up, w_down
    )
    mixer_out = mixer(
        queries, forget_pre, value_in, out_gate, lower_bound, out_gain, out_weight
    )
    return mixer_out, expert_out


def solution(mesh):
    split = Mesh(mesh.devices.reshape(8, 4, 2, mesh.shape["tp"]), ("ep_0", "ep_1", "ep_2", "tp"))
    placed = (
        P(EP, "tp"),
        P(EP, "tp"),
        P(EP, "tp"),
        P(EP, "tp"),
        P("tp"),
        P(),
        P("tp", None),
        P(EP, None),
        P(),
        P(EP, None),
        P(EP, None),
        P(EP, None, "tp"),
        P(EP, None, "tp"),
        P(EP, "tp", None),
    )
    return jax.shard_map(
        local,
        mesh=split,
        in_specs=placed,
        out_specs=(P(EP_TP, None), P(EP_TP, None)),
        check_vma=False,
    )
```

```python
import jax
import jax.numpy as jnp
from jax import lax
from jax.experimental import pallas as pl
from jax.experimental.pallas import tpu as pltpu
from jax.sharding import Mesh
from jax.sharding import PartitionSpec as P


HEAD_DIM = 128
BLOCK = 64
EP = ("ep_0", "ep_1", "ep_2")
EP_TP = ("ep_0", "ep_1", "ep_2", "tp")

EPS = 1e-06
HIGHEST = lax.Precision.HIGHEST


def rms_scale(values, gain):
    return values * lax.rsqrt(jnp.mean(values * values, axis=-1, keepdims=True) + EPS) * gain


def dot_nt(a, b, precision=HIGHEST):
    return lax.dot_general(
        a, b, (((1,), (1,)), ((), ())), precision=precision, preferred_element_type=jnp.float32
    )


def dot_tn(a, b, precision=HIGHEST):
    return lax.dot_general(
        a, b, (((0,), (0,)), ((), ())), precision=precision, preferred_element_type=jnp.float32
    )


def dot_nn(a, b, precision=HIGHEST):
    return lax.dot_general(
        a, b, (((1,), (0,)), ((), ())), precision=precision, preferred_element_type=jnp.float32
    )


def recurrence_kernel(q_ref, f_ref, v_ref, bound_ref, rec_ref, query_ref, state_ref, decay_ref):
    rows = q_ref.shape[0]
    row = lax.broadcasted_iota(jnp.int32, (BLOCK, BLOCK), 0)
    col = lax.broadcasted_iota(jnp.int32, (BLOCK, BLOCK), 1)
    causal = row >= col
    lower = causal.astype(jnp.float32)
    scale = 1.0 - bound_ref[0]

    def step(b, carry):
        state, before = carry
        here = pl.ds(pl.multiple_of(b * BLOCK, BLOCK), BLOCK)
        weight = scale * jax.nn.sigmoid(-f_ref[here, :])
        log_forget = jnp.log1p(-weight)
        cumulative = dot_nn(lower, log_forget)
        queries = q_ref[here, :].astype(jnp.float32)
        values = v_ref[here, :].astype(jnp.float32)
        decayed_query = queries * jnp.exp(cumulative)
        decayed_key = weight * jnp.exp(-cumulative)
        scores = jnp.where(causal, dot_nt(decayed_query, decayed_key), 0.0)
        rec_ref[here, :] = dot_nt(decayed_query, state) + dot_nn(scores, values)
        query_ref[here, :] = queries * jnp.exp(cumulative + before)
        total = cumulative[BLOCK - 1 :, :]
        state = jnp.exp(total) * state + dot_tn(values, weight * jnp.exp(total - cumulative))
        return state, before + total

    state, total = lax.fori_loop(
        0,
        rows // BLOCK,
        step,
        (jnp.zeros((HEAD_DIM, HEAD_DIM), jnp.float32), jnp.zeros((1, HEAD_DIM), jnp.float32)),
    )
    state_ref[0] = state
    decay_ref[0] = jnp.broadcast_to(jnp.exp(total), decay_ref.shape[1:])


def recurrence(queries, forget_pre, value_in, lower_bound):
    rows, width = queries.shape
    heads = width // HEAD_DIM
    wide = pl.BlockSpec((rows, HEAD_DIM), lambda h: (0, h))
    return pl.pallas_call(
        recurrence_kernel,
        grid=(heads,),
        in_specs=[wide, wide, wide, pl.BlockSpec((1, 1, HEAD_DIM), lambda h: (h, 0, 0))],
        out_specs=[
            wide,
            wide,
            pl.BlockSpec((1, HEAD_DIM, HEAD_DIM), lambda h: (h, 0, 0)),
            pl.BlockSpec((1, 8, HEAD_DIM), lambda h: (h, 0, 0)),
        ],
        out_shape=[
            jax.ShapeDtypeStruct((rows, width), jnp.float32),
            jax.ShapeDtypeStruct((rows, width), jnp.float32),
            jax.ShapeDtypeStruct((heads, HEAD_DIM, HEAD_DIM), jnp.float32),
            jax.ShapeDtypeStruct((heads, 8, HEAD_DIM), jnp.float32),
        ],
        name="recurrence",
    )(queries, forget_pre, value_in, lower_bound.reshape(heads, 1, HEAD_DIM))


def prefix_kernel(pieces_ref, out_ref):
    def step(k, before):
        out_ref[k] = before
        return before * pieces_ref[k, 8:, :] + pieces_ref[k, :8, :]

    lax.fori_loop(0, pieces_ref.shape[0], step, jnp.zeros(out_ref.shape[1:], jnp.float32))


def prefix(pieces):
    return pl.pallas_call(
        prefix_kernel,
        out_shape=jax.ShapeDtypeStruct((pieces.shape[0], 8, HEAD_DIM), jnp.float32),
        name="prefix",
    )(pieces)


def gate_kernel(rec_ref, query_ref, state_ref, out_gate_ref, gain_ref, out_ref):
    rec = rec_ref[...] + dot_nt(query_ref[...], state_ref[0])
    act = jax.nn.silu(out_gate_ref[...].astype(jnp.float32))
    out_ref[...] = (rms_scale(rec, gain_ref[...]) * act).astype(jnp.bfloat16)


def gate(rec, query, state, out_gate, out_gain):
    rows, width = rec.shape
    wide = pl.BlockSpec((rows, HEAD_DIM), lambda h: (0, h))
    return pl.pallas_call(
        gate_kernel,
        grid=(width // HEAD_DIM,),
        in_specs=[
            wide,
            wide,
            pl.BlockSpec((1, HEAD_DIM, HEAD_DIM), lambda h: (h, 0, 0)),
            wide,
            pl.BlockSpec((1, HEAD_DIM), lambda h: (0, 0)),
        ],
        out_specs=wide,
        out_shape=jax.ShapeDtypeStruct((rows, width), jnp.bfloat16),
        name="gate",
    )(rec, query, state, out_gate, out_gain.reshape(1, HEAD_DIM))


def mixer(queries, forget_pre, value_in, out_gate, lower_bound, out_gain, out_weight):
    heads = queries.shape[1] // HEAD_DIM
    spans = lax.axis_size(EP)
    lanes = lax.axis_size("tp")
    rec, query, state, decay = recurrence(queries, forget_pre, value_in, lower_bound)
    per_head = spans // heads
    decays = jnp.broadcast_to(decay[:, None], (heads, per_head, 8, HEAD_DIM))
    leaving = jnp.concatenate(
        [
            state.reshape(spans, heads * HEAD_DIM // spans, HEAD_DIM),
            decays.reshape(spans, 8, HEAD_DIM),
        ],
        axis=1,
    )
    pieces = lax.all_to_all(leaving, EP, split_axis=0, concat_axis=0, tiled=True)
    before = prefix(pieces)
    starts = lax.all_to_all(before, EP, split_axis=0, concat_axis=0, tiled=True)
    gated = gate(rec, query, starts.reshape(heads, HEAD_DIM, HEAD_DIM), out_gate, out_gain)
    parts = jnp.dot(gated, out_weight, preferred_element_type=jnp.float32).astype(jnp.bfloat16)
    lane = lax.axis_index("tp")
    share = parts.shape[0] // lanes
    total = None
    for by in range(lanes):
        part = lax.dynamic_slice_in_dim(parts, (lane + by) % lanes * share, share, 0)
        if by > 0:
            part = lax.ppermute(part, "tp", [(i, (i + by) % lanes) for i in range(lanes)])
        part = part.astype(jnp.float32)
        total = part if total is None else total + part
    return total.astype(jnp.bfloat16)


def expert_kernel(core_ref, *refs):
    sets, steps = 1, 4
    row_refs = refs[:sets]
    sources = refs[sets : sets + 4 * steps]
    out_refs = refs[sets + 4 * steps : 2 * sets + 4 * steps]
    in_buffer, out_buffer, sum_ref, sems = refs[2 * sets + 4 * steps :]
    rows = row_refs[0].shape[0]
    half = out_buffer.shape[2]

    def copy(step, kind):
        buffer = in_buffer if kind < 2 else out_buffer
        place = 2 * step + kind % 2
        return pltpu.make_async_copy(
            sources[kind * steps + step], buffer.at[place], sems.at[4 * step + kind]
        )

    for step in range(steps):
        for kind in range(4):
            copy(step, kind).start()
    gate_is_own = core_ref[0] == 0
    for step in range(steps):
        for kind in range(4):
            copy(step, kind).wait()
        for s in range(sets):
            here = slice(s * rows, (s + 1) * rows)
            own = dot_nn(row_refs[s][...], in_buffer[2 * step], None)
            other = dot_nn(row_refs[s][...], in_buffer[2 * step + 1], None)
            gate_pre = jnp.where(gate_is_own, own, other)
            up_pre = jnp.where(gate_is_own, other, own)
            hidden = (jax.nn.silu(gate_pre) * up_pre).astype(jnp.bfloat16)
            for side in range(2):
                part = dot_nn(hidden, out_buffer[2 * step + side], None)
                if step > 0:
                    part = part + sum_ref[side, here, :]
                sum_ref[side, here, :] = part
    for s in range(sets):
        here = slice(s * rows, (s + 1) * rows)
        for side in range(2):
            place = (core_ref[0] if side == 0 else 1 - core_ref[0]) * half
            out_refs[s][:, pl.ds(pl.multiple_of(place, half), half)] = sum_ref[
                side, here, :
            ].astype(jnp.bfloat16)


def expert_rows(core, row_set, own_in, other_in, own_out, other_out):
    rows, width = row_set.shape
    units = own_in[0].shape[1]
    half = own_out[0].shape[1]
    vmem = pl.BlockSpec(memory_space=pltpu.VMEM)
    hbm = pl.BlockSpec(memory_space=pl.ANY)
    return pl.pallas_call(
        expert_kernel,
        in_specs=[pl.BlockSpec(memory_space=pltpu.SMEM), vmem] + [hbm] * 16,
        out_specs=vmem,
        out_shape=jax.ShapeDtypeStruct((rows, width), jnp.bfloat16),
        scratch_shapes=[
            pltpu.VMEM((8, width, units), jnp.bfloat16),
            pltpu.VMEM((8, units, half), jnp.bfloat16),
            pltpu.VMEM((2, rows, half), jnp.float32),
            pltpu.SemaphoreType.DMA((16,)),
        ],
        cost_estimate=pl.CostEstimate(
            flops=6 * rows * width * 1024, bytes_accessed=16 * 2**20, transcendentals=0
        ),
        name="expert_rows",
    )(core, row_set, *own_in, *other_in, *own_out, *other_out)


def slot_places(slot_count):
    slot = jnp.arange(slot_count, dtype=jnp.int32)
    device, place = slot // 2, slot % 2
    expert = device // 8 * 4 + device % 4
    return expert, device // 4 % 2 * 2 + place


def slots_filled(ids, slot_count):
    expert, rank = slot_places(slot_count)
    named = jnp.any(ids.T[:, None, :] == expert[None, :, None], axis=0)
    order = jnp.arange(ids.shape[0], dtype=jnp.int32)
    earlier = (order[:, None] < order[None, :]).astype(jnp.bfloat16)
    ranks = jnp.dot(named.astype(jnp.bfloat16), earlier, preferred_element_type=jnp.float32)
    return named & (ranks == rank.astype(jnp.float32)[:, None])


def slot_weights(ids, weights, slot_count):
    expert, rank = slot_places(slot_count)
    named = ids[:, :, None] == expert[None, None, :]
    weight = jnp.sum(jnp.where(named, weights[:, :, None], 0.0), axis=1)
    named = jnp.any(named, axis=1)
    order = jnp.arange(ids.shape[0], dtype=jnp.int32)
    earlier = (order[None, :] < order[:, None]).astype(jnp.bfloat16)
    ranks = jnp.dot(earlier, named.astype(jnp.bfloat16), preferred_element_type=jnp.float32)
    return jnp.where(ranks == rank.astype(jnp.float32)[None, :], weight, 0.0)


def weight_moves(turn):
    moves = []
    for core in range(2):
        for lane in range(4):
            piece = lane ^ turn
            moves.append((core * 4 + lane, (piece % 2) * 4 + 2 * core + piece // 2))
    return moves


RING = ("ep_2", "tp")


def experts(moe_tokens, moe_gain, expert_ids, route_weights, w_gate, w_up, w_down):
    lanes = lax.axis_size("tp")
    lane = lax.axis_index("tp")
    core = lax.axis_index("ep_2")
    devices = lax.axis_size(EP_TP)
    model_width = w_gate.shape[1]
    qrows = moe_tokens.shape[0] // lanes
    slots = 2 * devices
    half = model_width // 2

    own_in, own_out, other_in, other_out = [], [], [], []
    for turn in range(4):
        piece = lane ^ turn
        expert, part = piece // 2, piece % 2
        gate_now = lax.dynamic_index_in_dim(w_gate, expert, 0, keepdims=False)
        up_now = lax.dynamic_index_in_dim(w_up, expert, 0, keepdims=False)
        in_now = jnp.where(part == 0, gate_now, up_now)
        down_now = lax.dynamic_slice(
            w_down, (expert, 0, part * half), (1, w_down.shape[1], half)
        )[0]
        own_in.append(lax.ppermute(in_now, RING, weight_moves(turn)))
        own_out.append(lax.ppermute(down_now, RING, weight_moves(turn)))
    for turn in range(4):
        other_in.append(lax.ppermute(own_in[turn ^ 1], "ep_2", [(0, 1), (1, 0)]))
        other_out.append(lax.ppermute(own_out[turn ^ 1], "ep_2", [(0, 1), (1, 0)]))

    start = lane * qrows
    ids = lax.dynamic_slice_in_dim(expert_ids, start, qrows, 0)
    weights = lax.dynamic_slice_in_dim(route_weights, start, qrows, 0)
    tokens = lax.dynamic_slice_in_dim(moe_tokens, start, qrows, 0)
    normed = rms_scale(tokens.astype(jnp.float32), moe_gain).astype(jnp.bfloat16)
    filled = slots_filled(ids, slots).astype(jnp.bfloat16)
    leaving = jnp.dot(filled, normed, preferred_element_type=jnp.float32).astype(jnp.bfloat16)
    arrived = lax.all_to_all(
        leaving.reshape(devices, 2, model_width), EP_TP, 0, 0, tiled=True
    )

    results = expert_rows(
        core.astype(jnp.int32).reshape(1),
        arrived.reshape(slots, model_width),
        own_in,
        other_in,
        own_out,
        other_out,
    )

    returned = lax.all_to_all(
        results.reshape(devices, 2, model_width), EP_TP, 0, 0, tiled=True
    )
    returned = returned.reshape(slots, model_width)
    mix = slot_weights(ids, weights, slots)
    high = lax.reduce_precision(mix, 8, 7)
    out = jnp.dot(high.astype(jnp.bfloat16), returned, preferred_element_type=jnp.float32)
    out += jnp.dot(
        (mix - high).astype(jnp.bfloat16), returned, preferred_element_type=jnp.float32
    )
    return out.astype(jnp.bfloat16)


def local(
    queries,
    forget_pre,
    value_in,
    out_gate,
    lower_bound,
    out_gain,
    out_weight,
    moe_tokens,
    moe_gain,
    expert_ids,
    route_weights,
    w_gate,
    w_up,
    w_down,
):
    expert_out = experts(
        moe_tokens, moe_gain, expert_ids, route_weights, w_gate, w_up, w_down
    )
    mixer_out = mixer(queries, forget_pre, value_in, out_gate, lower_bound, out_gain, out_weight)
    return mixer_out, expert_out


def solution(mesh):
    split = Mesh(mesh.devices.reshape(8, 4, 2, mesh.shape["tp"]), ("ep_0", "ep_1", "ep_2", "tp"))
    placed = (
        P(EP, "tp"),
        P(EP, "tp"),
        P(EP, "tp"),
        P(EP, "tp"),
        P("tp"),
        P(),
        P("tp", None),
        P(EP, None),
        P(),
        P(EP, None),
        P(EP, None),
        P(EP, None, "tp"),
        P(EP, None, "tp"),
        P(EP, "tp", None),
    )
    return jax.shard_map(
        local,
        mesh=split,
        in_specs=placed,
        out_specs=(P(EP_TP, None), P(EP_TP, None)),
        check_vma=False,
    )
```

```python
import jax
import jax.numpy as jnp
from jax import lax
from jax.experimental import pallas as pl
from jax.experimental.pallas import tpu as pltpu
from jax.sharding import Mesh
from jax.sharding import PartitionSpec as P


HEAD_DIM = 128
BLOCK = 64
EP = ("ep_0", "ep_1", "ep_2")
EP_TP = ("ep_0", "ep_1", "ep_2", "tp")

EPS = 1e-06
HIGHEST = lax.Precision.HIGHEST


def rms_scale(values, gain):
    return values * lax.rsqrt(jnp.mean(values * values, axis=-1, keepdims=True) + EPS) * gain


def dot_nt(a, b, precision=HIGHEST):
    return lax.dot_general(
        a, b, (((1,), (1,)), ((), ())), precision=precision, preferred_element_type=jnp.float32
    )


def dot_tn(a, b, precision=HIGHEST):
    return lax.dot_general(
        a, b, (((0,), (0,)), ((), ())), precision=precision, preferred_element_type=jnp.float32
    )


def dot_nn(a, b, precision=HIGHEST):
    return lax.dot_general(
        a, b, (((1,), (0,)), ((), ())), precision=precision, preferred_element_type=jnp.float32
    )


def recurrence_kernel(q_ref, f_ref, v_ref, bound_ref, rec_ref, query_ref, state_ref, decay_ref):
    rows = q_ref.shape[0]
    row = lax.broadcasted_iota(jnp.int32, (BLOCK, BLOCK), 0)
    col = lax.broadcasted_iota(jnp.int32, (BLOCK, BLOCK), 1)
    causal = row >= col
    lower = causal.astype(jnp.float32)
    scale = 1.0 - bound_ref[0]

    def step(b, carry):
        state, before = carry
        here = pl.ds(pl.multiple_of(b * BLOCK, BLOCK), BLOCK)
        weight = scale * jax.nn.sigmoid(-f_ref[here, :])
        log_forget = jnp.log1p(-weight)
        cumulative = dot_nn(lower, log_forget)
        queries = q_ref[here, :].astype(jnp.float32)
        values = v_ref[here, :].astype(jnp.float32)
        decayed_query = queries * jnp.exp(cumulative)
        decayed_key = weight * jnp.exp(-cumulative)
        scores = jnp.where(causal, dot_nt(decayed_query, decayed_key), 0.0)
        rec_ref[here, :] = dot_nt(decayed_query, state) + dot_nn(scores, values)
        query_ref[here, :] = queries * jnp.exp(cumulative + before)
        total = cumulative[BLOCK - 1 :, :]
        state = jnp.exp(total) * state + dot_tn(values, weight * jnp.exp(total - cumulative))
        return state, before + total

    state, total = lax.fori_loop(
        0,
        rows // BLOCK,
        step,
        (jnp.zeros((HEAD_DIM, HEAD_DIM), jnp.float32), jnp.zeros((1, HEAD_DIM), jnp.float32)),
    )
    state_ref[0] = state
    decay_ref[0] = jnp.broadcast_to(jnp.exp(total), decay_ref.shape[1:])


def recurrence(queries, forget_pre, value_in, lower_bound):
    rows, width = queries.shape
    heads = width // HEAD_DIM
    wide = pl.BlockSpec((rows, HEAD_DIM), lambda h: (0, h))
    return pl.pallas_call(
        recurrence_kernel,
        grid=(heads,),
        in_specs=[wide, wide, wide, pl.BlockSpec((1, 1, HEAD_DIM), lambda h: (h, 0, 0))],
        out_specs=[
            wide,
            wide,
            pl.BlockSpec((1, HEAD_DIM, HEAD_DIM), lambda h: (h, 0, 0)),
            pl.BlockSpec((1, 8, HEAD_DIM), lambda h: (h, 0, 0)),
        ],
        out_shape=[
            jax.ShapeDtypeStruct((rows, width), jnp.float32),
            jax.ShapeDtypeStruct((rows, width), jnp.float32),
            jax.ShapeDtypeStruct((heads, HEAD_DIM, HEAD_DIM), jnp.float32),
            jax.ShapeDtypeStruct((heads, 8, HEAD_DIM), jnp.float32),
        ],
        name="recurrence",
    )(queries, forget_pre, value_in, lower_bound.reshape(heads, 1, HEAD_DIM))


def prefix_kernel(pieces_ref, out_ref):
    def step(k, before):
        out_ref[k] = before
        return before * pieces_ref[k, 8:, :] + pieces_ref[k, :8, :]

    lax.fori_loop(0, pieces_ref.shape[0], step, jnp.zeros(out_ref.shape[1:], jnp.float32))


def prefix(pieces):
    return pl.pallas_call(
        prefix_kernel,
        out_shape=jax.ShapeDtypeStruct((pieces.shape[0], 8, HEAD_DIM), jnp.float32),
        name="prefix",
    )(pieces)


def gate_kernel(rec_ref, query_ref, state_ref, out_gate_ref, gain_ref, out_ref):
    rec = rec_ref[...] + dot_nt(query_ref[...], state_ref[0])
    act = jax.nn.silu(out_gate_ref[...].astype(jnp.float32))
    out_ref[...] = (rms_scale(rec, gain_ref[...]) * act).astype(jnp.bfloat16)


def gate(rec, query, state, out_gate, out_gain):
    rows, width = rec.shape
    wide = pl.BlockSpec((rows, HEAD_DIM), lambda h: (0, h))
    return pl.pallas_call(
        gate_kernel,
        grid=(width // HEAD_DIM,),
        in_specs=[
            wide,
            wide,
            pl.BlockSpec((1, HEAD_DIM, HEAD_DIM), lambda h: (h, 0, 0)),
            wide,
            pl.BlockSpec((1, HEAD_DIM), lambda h: (0, 0)),
        ],
        out_specs=wide,
        out_shape=jax.ShapeDtypeStruct((rows, width), jnp.bfloat16),
        name="gate",
    )(rec, query, state, out_gate, out_gain.reshape(1, HEAD_DIM))


def mixer(queries, forget_pre, value_in, out_gate, lower_bound, out_gain, out_weight):
    heads = queries.shape[1] // HEAD_DIM
    spans = lax.axis_size(EP)
    lanes = lax.axis_size("tp")
    rec, query, state, decay = recurrence(queries, forget_pre, value_in, lower_bound)
    per_head = spans // heads
    decays = jnp.broadcast_to(decay[:, None], (heads, per_head, 8, HEAD_DIM))
    leaving = jnp.concatenate(
        [
            state.reshape(spans, heads * HEAD_DIM // spans, HEAD_DIM),
            decays.reshape(spans, 8, HEAD_DIM),
        ],
        axis=1,
    )
    pieces = lax.all_to_all(leaving, EP, split_axis=0, concat_axis=0, tiled=True)
    before = prefix(pieces)
    starts = lax.all_to_all(before, EP, split_axis=0, concat_axis=0, tiled=True)
    gated = gate(rec, query, starts.reshape(heads, HEAD_DIM, HEAD_DIM), out_gate, out_gain)
    parts = jnp.dot(gated, out_weight, preferred_element_type=jnp.float32).astype(jnp.bfloat16)
    lane = lax.axis_index("tp")
    share = parts.shape[0] // lanes
    total = None
    for by in range(lanes):
        part = lax.dynamic_slice_in_dim(parts, (lane + by) % lanes * share, share, 0)
        if by > 0:
            part = lax.ppermute(part, "tp", [(i, (i + by) % lanes) for i in range(lanes)])
        part = part.astype(jnp.float32)
        total = part if total is None else total + part
    return total.astype(jnp.bfloat16)


STEPS = 4


def expert_kernel(core_ref, row_ref, *refs):
    sources = refs[: 2 * STEPS]
    out_ref, weight_ref, sems = refs[2 * STEPS :]
    width = row_ref.shape[1]
    units = weight_ref.shape[2]
    half = width // 2

    def copy(place):
        return pltpu.make_async_copy(sources[place], weight_ref.at[place], sems.at[place])

    for place in range(2 * STEPS):
        copy(place).start()
    gate_is_own = core_ref[0] == 0
    hidden = []
    for step in range(STEPS):
        products = []
        for side in range(2):
            copy(2 * step + side).wait()
            products.append(dot_nn(row_ref[...], weight_ref[2 * step + side, :width, :], None))
        own, other = products
        gate_pre = jnp.where(gate_is_own, own, other)
        up_pre = jnp.where(gate_is_own, other, own)
        hidden.append((jax.nn.silu(gate_pre) * up_pre).astype(jnp.bfloat16))
    for side in range(2):
        place = (core_ref[0] if side == 0 else 1 - core_ref[0]) * half
        for block in range(half // units):
            top = width + block * units
            total = None
            for step in range(STEPS):
                part = dot_nn(hidden[step], weight_ref[2 * step + side, top : top + units, :], None)
                total = part if total is None else total + part
            here = pl.ds(pl.multiple_of(place + block * units, units), units)
            out_ref[:, here] = total.astype(jnp.bfloat16)


def expert_rows(core, row_set, own, other):
    rows, width = row_set.shape
    units = own[0].shape[1]
    vmem = pl.BlockSpec(memory_space=pltpu.VMEM)
    hbm = pl.BlockSpec(memory_space=pl.ANY)
    return pl.pallas_call(
        expert_kernel,
        in_specs=[pl.BlockSpec(memory_space=pltpu.SMEM), vmem] + [hbm] * (2 * STEPS),
        out_specs=vmem,
        out_shape=jax.ShapeDtypeStruct((rows, width), jnp.bfloat16),
        scratch_shapes=[
            pltpu.VMEM((2 * STEPS, *own[0].shape), jnp.bfloat16),
            pltpu.SemaphoreType.DMA((2 * STEPS,)),
        ],
        cost_estimate=pl.CostEstimate(
            flops=6 * rows * width * units * STEPS,
            bytes_accessed=16 * 2**20,
            transcendentals=rows * units * STEPS,
        ),
        name="expert_rows",
    )(core, row_set, *[piece for pair in zip(own, other) for piece in pair])


def slot_places(slot_count):
    slot = jnp.arange(slot_count, dtype=jnp.int32)
    device, place = slot // 2, slot % 2
    expert = device // 8 * 4 + device % 4
    return expert, device // 4 % 2 * 2 + place


def slots_filled(ids, slot_count):
    expert, rank = slot_places(slot_count)
    named = jnp.any(ids.T[:, None, :] == expert[None, :, None], axis=0)
    order = jnp.arange(ids.shape[0], dtype=jnp.int32)
    earlier = (order[:, None] < order[None, :]).astype(jnp.bfloat16)
    ranks = jnp.dot(named.astype(jnp.bfloat16), earlier, preferred_element_type=jnp.float32)
    return named & (ranks == rank.astype(jnp.float32)[:, None])


def slot_weights(ids, weights, slot_count):
    expert, rank = slot_places(slot_count)
    named = ids[:, :, None] == expert[None, None, :]
    weight = jnp.sum(jnp.where(named, weights[:, :, None], 0.0), axis=1)
    named = jnp.any(named, axis=1)
    order = jnp.arange(ids.shape[0], dtype=jnp.int32)
    earlier = (order[None, :] < order[:, None]).astype(jnp.bfloat16)
    ranks = jnp.dot(earlier, named.astype(jnp.bfloat16), preferred_element_type=jnp.float32)
    return jnp.where(ranks == rank.astype(jnp.float32)[None, :], weight, 0.0)


def weight_moves(turn):
    moves = []
    for core in range(2):
        for lane in range(4):
            piece = lane ^ turn
            moves.append((core * 4 + lane, (piece % 2) * 4 + 2 * core + piece // 2))
    return moves


RING = ("ep_2", "tp")


def experts(moe_tokens, moe_gain, expert_ids, route_weights, w_gate, w_up, w_down):
    lanes = lax.axis_size("tp")
    lane = lax.axis_index("tp")
    core = lax.axis_index("ep_2")
    devices = lax.axis_size(EP_TP)
    model_width = w_gate.shape[1]
    qrows = moe_tokens.shape[0] // lanes
    slots = 2 * devices
    half = model_width // 2

    own = []
    for turn in range(STEPS):
        piece = lane ^ turn
        expert, part = piece // 2, piece % 2
        gate_now = lax.dynamic_index_in_dim(w_gate, expert, 0, keepdims=False)
        up_now = lax.dynamic_index_in_dim(w_up, expert, 0, keepdims=False)
        in_now = jnp.where(part == 0, gate_now, up_now)
        units = in_now.shape[1]
        blocks = [
            lax.dynamic_slice(w_down, (expert, 0, part * half + k), (1, units, units))[0]
            for k in range(0, half, units)
        ]
        leaving = jnp.concatenate([in_now] + blocks, axis=0)
        own.append(lax.ppermute(leaving, RING, weight_moves(turn)))
    other = []
    for turn in range(STEPS):
        other.append(lax.ppermute(own[turn ^ 1], "ep_2", [(0, 1), (1, 0)]))

    start = lane * qrows
    ids = lax.dynamic_slice_in_dim(expert_ids, start, qrows, 0)
    weights = lax.dynamic_slice_in_dim(route_weights, start, qrows, 0)
    tokens = lax.dynamic_slice_in_dim(moe_tokens, start, qrows, 0)
    normed = rms_scale(tokens.astype(jnp.float32), moe_gain).astype(jnp.bfloat16)
    filled = slots_filled(ids, slots).astype(jnp.bfloat16)
    leaving = jnp.dot(filled, normed, preferred_element_type=jnp.float32).astype(jnp.bfloat16)
    arrived = lax.all_to_all(
        leaving.reshape(devices, 2, model_width), EP_TP, 0, 0, tiled=True
    )

    results = expert_rows(
        core.astype(jnp.int32).reshape(1),
        arrived.reshape(slots, model_width),
        own,
        other,
    )

    returned = lax.all_to_all(
        results.reshape(devices, 2, model_width), EP_TP, 0, 0, tiled=True
    )
    returned = returned.reshape(slots, model_width)
    mix = slot_weights(ids, weights, slots)
    high = lax.reduce_precision(mix, 8, 7)
    factors = jnp.concatenate([high, mix - high], axis=0).astype(jnp.bfloat16)
    sums = jnp.dot(factors, returned, preferred_element_type=jnp.float32)
    return (sums[:qrows] + sums[qrows:]).astype(jnp.bfloat16)


def local(
    queries,
    forget_pre,
    value_in,
    out_gate,
    lower_bound,
    out_gain,
    out_weight,
    moe_tokens,
    moe_gain,
    expert_ids,
    route_weights,
    w_gate,
    w_up,
    w_down,
):
    expert_out = experts(
        moe_tokens, moe_gain, expert_ids, route_weights, w_gate, w_up, w_down
    )
    mixer_out = mixer(queries, forget_pre, value_in, out_gate, lower_bound, out_gain, out_weight)
    return mixer_out, expert_out


def solution(mesh):
    split = Mesh(mesh.devices.reshape(8, 4, 2, mesh.shape["tp"]), ("ep_0", "ep_1", "ep_2", "tp"))
    placed = (
        P(EP, "tp"),
        P(EP, "tp"),
        P(EP, "tp"),
        P(EP, "tp"),
        P("tp"),
        P(),
        P("tp", None),
        P(EP, None),
        P(),
        P(EP, None),
        P(EP, None),
        P(EP, None, "tp"),
        P(EP, None, "tp"),
        P(EP, "tp", None),
    )
    return jax.shard_map(
        local,
        mesh=split,
        in_specs=placed,
        out_specs=(P(EP_TP, None), P(EP_TP, None)),
        check_vma=False,
    )
```
